32 devices in a mesh: grp: 2 (over y), tp: 4 (over z), dp: 4 (over x, core).
Axes of the slice: x: 2, y: 2, z: 4, core: 2. Of those that a mesh axis runs over, the one named last changes fastest.
Arguments:
- skip_path_activations: bfloat16 [128, 8, 4096], P('grp', None, 'dp'), parts along dimension 0
- novel_lengths_per_sequence: int32 [128], P(('grp', 'dp')), parts along dimension 0, may hold values from 1 to 8, 256 in all
- input_normalizer_scales: bfloat16 [2, 4096], P(None, 'dp'), may hold values from 0.099609375 to 1.8984375
- question_projector: bfloat16 [2, 4096, 2048], P(None, 'dp', 'tp'), may hold values from -0.09375 to 0.09375
- lookup_projector: bfloat16 [2, 4096, 2048], P(None, 'dp', 'tp'), may hold values from -0.09375 to 0.09375
- payload_projector: bfloat16 [2, 4096, 4096], P(None, 'dp', 'tp'), may hold values from -0.09375 to 0.09375
- emitted_valve_projector: bfloat16 [2, 4096, 4096], P(None, 'dp', 'tp'), may hold values from -0.09375 to 0.09375
- keeping_valve_projector: bfloat16 [2, 4096, 2048], P(None, 'dp', 'tp'), may hold values from -0.09375 to 0.09375
- keeping_valve_shift: float32 [2, 2048], P(None, 'tp'), may hold values from -3 to 6
- additional_dwindle_exponent: float32 [128, 8, 16], P(('grp', 'dp'), None, 'tp'), parts along dimension 0, may hold values from -0.7 to 0
- headwise_normalizer_scales: bfloat16 [2, 256], replicated, may hold values from 0.099609375 to 1.8984375
- closing_projector: bfloat16 [2, 4096, 4096], P(None, 'tp', 'dp'), may hold values from -0.1875 to 0.1875
- earlier_recurrence_grid: float32 [2, 128, 16, 128, 256], P(None, ('grp', 'dp'), 'tp'), parts along dimension 1, may hold values from -6 to 6
Outputs:
- stream_out: bfloat16 [128, 8, 4096], P('grp', None, 'dp'), parts along dimension 0
- state_out: float32 [2, 128, 16, 128, 256], P(None, ('grp', 'dp'), 'tp'), parts along dimension 1
The draws below stay inside these ranges and needn't reach their ends.
There are 2 independent parts, one for each index of `grp`. The reference program is written for one: setup_inputs(seed, part) draws one part's arguments, and reference() takes and returns one part's arrays. A program takes and returns all parts, laid end to end along the dimension named above; an argument that names none is the same for every part. Nothing has to cross between parts.
Inputs may be any that keep to these rules, and one draw needn't show every extreme that they name: `novel_lengths_per_sequence`: each sequence has 1 to 8 live token slots, the first ones; some sequence has 8. In each group the live slots of its 64 sequences add up to half of 64 times 8.
All inputs are finite; a program needn't handle non-finite values.
Results may differ from the reference program's by a relative error of at most 0.024.
Values may be sent and summed in bfloat16 or wider, within the bound.
A program may use at most 128 MiB of HBM per device.

```python
import math
import jax
import jax.numpy as jnp
import numpy as np
from jax import lax

MODEL_BREADTH = 4096
HEADS = 16
DK = 128
DV = 256
LAYERS = 2
NEW = 8
QK = 2048
VW = 4096
BATCH = 64
N_DP = 4


def draw_skip_path_activations(key, part):
    first = jax.random.fold_in(jax.random.fold_in(key, 11), 0)
    column_scale = 0.5 * 10.0 ** (jnp.arange(MODEL_BREADTH, dtype=jnp.float32) / MODEL_BREADTH)
    values = jnp.clip(jax.random.normal(first, (BATCH, NEW, MODEL_BREADTH), jnp.float32), -6.0, 6.0) * column_scale
    return values.astype(jnp.bfloat16)


def draw_keeping_valve_shift(key, part):
    first, second, third = jax.random.split(jax.random.fold_in(key, 23), 3)
    share = 0.5
    quick = jax.random.uniform(first, (LAYERS, QK), jnp.float32) < share
    quick_value = jax.random.uniform(second, (LAYERS, QK), jnp.float32, -3.0, 0.0)
    slow_value = jax.random.uniform(third, (LAYERS, QK), jnp.float32, 2.0, 6.0)
    return jnp.where(quick, quick_value, slow_value)


def draw_additional_dwindle_exponent(key, part):
    first, second = jax.random.split(jax.random.fold_in(key, 37))
    hit = jax.random.randint(first, (BATCH, NEW, HEADS), 0, 12) == 0
    amount = jnp.log(jax.random.uniform(second, (BATCH, NEW, HEADS), jnp.float32, 0.5, 0.8))
    return jnp.where(hit, amount, 0.0).astype(jnp.float32)


def levels(stream_key, extent, cuts, smallest, high):
    def one(axis_at, blocks):
        draws = jax.random.uniform(jax.random.fold_in(jax.random.fold_in(stream_key, 6), axis_at), (blocks,), jnp.float32, smallest / len(cuts), high / len(cuts))
        return jnp.repeat(jnp.exp(draws), extent[axis_at] // blocks).reshape((-1,) + (1,) * (len(extent) - axis_at - 1))

    factor_of = one(*cuts[0])
    for cut in cuts[1:]:
        factor_of = factor_of * one(*cut)
    return factor_of


def split_up(number_of, total, bound, lean):
    weights = [(1 << 20) // math.isqrt(grade ** lean) + 1 for grade in range(2, number_of + 1)]
    rest, given = total - bound - (number_of - 1), [1] * (number_of - 1)
    while rest > 0:
        movable = [i for i in range(number_of - 1) if given[i] < bound]
        mass, left = sum([weights[i] for i in movable]), rest
        for i in movable:
            addition = min(bound - given[i], max(1, left * weights[i] // mass), rest)
            given[i] = given[i] + addition
            rest = rest - addition
    return np.array([bound] + given)


def ragged(rng, number_of, total, reach, slope):
    if number_of == 2:
        one = jax.random.randint(rng, (), max(1, total - reach), min(reach, total - 1) + 1)
        return jnp.stack([one, total - one])
    lengths = jnp.asarray(split_up(number_of, total, reach, slope), jnp.int32)
    couples = (number_of - 1) // 2
    source_of, receiver = lengths[1:1 + 2 * couples:2], lengths[2:2 + 2 * couples:2]
    slack = jnp.minimum(source_of - 1, reach - receiver)
    passed = jax.random.randint(jax.random.fold_in(rng, 1), (couples,), 0, 1 << 20) % (slack + 1)
    lengths = lengths.at[1:1 + 2 * couples:2].set(source_of - passed).at[2:2 + 2 * couples:2].set(receiver + passed)
    return lengths[jax.random.permutation(jax.random.fold_in(rng, 2), number_of)]


def noise(stream_key, shape, scale, bound, shards=(), kind=jnp.bfloat16):
    array = scale * jax.random.normal(stream_key, shape, jnp.float32)
    if shards:
        array = array * levels(stream_key, shape, shards, -0.22, 0.18)
    return jnp.clip(array, -bound, bound).astype(kind)


def setup_inputs(seed: int = 0, part: int = 0) -> dict:
    arg_keys = jax.random.split(jax.random.key(seed), 14)
    part_keys = jax.random.split(jax.random.fold_in(arg_keys[13], part), 14)
    skip_path_activations = draw_skip_path_activations(jax.random.fold_in(jax.random.fold_in(arg_keys[13], part), 71), part)
    novel_lengths_per_sequence = ragged(part_keys[1], BATCH, BATCH * NEW // 2, NEW, 2).astype(jnp.int32)
    input_normalizer_scales = jnp.clip(1.0 + 0.18 * jax.random.normal(arg_keys[2], (LAYERS, MODEL_BREADTH), jnp.float32), 0.099609375, 1.8984375).astype(jnp.bfloat16)
    question_projector = noise(arg_keys[3], (LAYERS, MODEL_BREADTH, QK), MODEL_BREADTH ** -0.5, 0.09375, ((1, 4), (2, 4)))
    lookup_projector = noise(arg_keys[4], (LAYERS, MODEL_BREADTH, QK), MODEL_BREADTH ** -0.5, 0.09375, ((1, 4), (2, 4)))
    payload_projector = noise(arg_keys[5], (LAYERS, MODEL_BREADTH, VW), MODEL_BREADTH ** -0.5, 0.09375, ((1, 4), (2, 4)))
    emitted_valve_projector = noise(arg_keys[6], (LAYERS, MODEL_BREADTH, VW), MODEL_BREADTH ** -0.5, 0.09375, ((1, 4), (2, 4)))
    keeping_valve_projector = noise(arg_keys[7], (LAYERS, MODEL_BREADTH, QK), MODEL_BREADTH ** -0.5, 0.09375, ((1, 4), (2, 4)))
    keeping_valve_shift = draw_keeping_valve_shift(jax.random.fold_in(arg_keys[13], 71), part)
    additional_dwindle_exponent = draw_additional_dwindle_exponent(jax.random.fold_in(jax.random.fold_in(arg_keys[13], part), 71), part)
    headwise_normalizer_scales = jnp.clip(1.0 + 0.18 * jax.random.normal(arg_keys[10], (LAYERS, DV), jnp.float32), 0.099609375, 1.8984375).astype(jnp.bfloat16)
    closing_projector = noise(arg_keys[11], (LAYERS, VW, MODEL_BREADTH), (VW // 4) ** -0.5, 0.1875, ((1, 4), (2, 4)))
    earlier_recurrence_grid = noise(part_keys[12], (LAYERS, BATCH, HEADS, DK, DV), 1.0, 6.0, ((1, 4), (2, 4)), jnp.float32)
    return {"skip_path_activations": skip_path_activations, "novel_lengths_per_sequence": novel_lengths_per_sequence, "input_normalizer_scales": input_normalizer_scales, "question_projector": question_projector, "lookup_projector": lookup_projector, "payload_projector": payload_projector, "emitted_valve_projector": emitted_valve_projector, "keeping_valve_projector": keeping_valve_projector, "keeping_valve_shift": keeping_valve_shift, "additional_dwindle_exponent": additional_dwindle_exponent, "headwise_normalizer_scales": headwise_normalizer_scales, "closing_projector": closing_projector, "earlier_recurrence_grid": earlier_recurrence_grid}


EPS = 1e-06
TAU = 16.0

def scaled_rms(values_f, gain):
    return values_f * lax.rsqrt(lax.optimization_barrier(jnp.mean(values_f * values_f, axis=-1, keepdims=True)) + EPS) * gain.astype(jnp.float32)

def round_trip(values_f):
    return lax.optimization_barrier(values_f.astype(jnp.bfloat16)).astype(jnp.float32)

def split_dot(normed, weight):
    number_of_lines = normed.shape[0]
    blocks = normed.astype(jnp.float32).reshape(number_of_lines, N_DP, MODEL_BREADTH // N_DP)
    pieces = weight.astype(jnp.float32).reshape(N_DP, MODEL_BREADTH // N_DP, weight.shape[1])
    partial_value = jnp.einsum('rnk,nkc->nrc', blocks, pieces, precision=lax.Precision.HIGHEST)
    return round_trip(partial_value).sum(axis=0)

def advance(query_rows, key_rows, value_rows, fade_log_amount, carried):
    steps_n = query_rows.shape[1]
    cumulative = jnp.cumsum(fade_log_amount, axis=1)
    spread = cumulative[:, :, None] - cumulative[:, None, :]
    causal = jnp.tril(jnp.ones((steps_n, steps_n), dtype=bool))
    decay_mat = jnp.exp(jnp.where(causal[None, :, :, None, None], spread, -jnp.inf))
    scores = jnp.einsum('sihd,sjhd,sijhd->shij', query_rows, key_rows, decay_mat, precision=lax.Precision.HIGHEST)
    within = jnp.einsum('shij,sjhv->sihv', scores, value_rows, precision=lax.Precision.HIGHEST)
    carried_part = jnp.einsum('sihd,shdv->sihv', query_rows * jnp.exp(cumulative), carried, precision=lax.Precision.HIGHEST)
    final_log = cumulative[:, -1]
    weighted = key_rows * jnp.exp(final_log[:, None] - cumulative)
    updated = jnp.exp(final_log)[..., None] * carried + jnp.einsum('sjhd,sjhv->shdv', weighted, value_rows, precision=lax.Precision.HIGHEST)
    return (within + carried_part, updated)

def reference(skip_path_activations, novel_lengths_per_sequence, input_normalizer_scales, question_projector, lookup_projector, payload_projector, emitted_valve_projector, keeping_valve_projector, keeping_valve_shift, additional_dwindle_exponent, headwise_normalizer_scales, closing_projector, earlier_recurrence_grid):
    number_of_lines = BATCH * NEW
    ongoing = skip_path_activations.reshape(number_of_lines, MODEL_BREADTH)
    live_entry_indicator = (jnp.arange(NEW, dtype=jnp.int32)[None, :] < novel_lengths_per_sequence[:, None]).astype(jnp.float32)
    new_states = []
    for block_index in range(LAYERS):
        normed = scaled_rms(ongoing.astype(jnp.float32), input_normalizer_scales[block_index]).astype(jnp.bfloat16)
        query_rows = round_trip(split_dot(normed, question_projector[block_index])) * DK ** (-0.5)
        key_rows = round_trip(split_dot(normed, lookup_projector[block_index]))
        value_rows = round_trip(split_dot(normed, payload_projector[block_index]))
        gate_rows = round_trip(split_dot(normed, emitted_valve_projector[block_index]))
        logits = split_dot(normed, keeping_valve_projector[block_index])
        fade_log_amount = (jax.nn.log_sigmoid(logits + keeping_valve_shift[block_index]) / TAU).reshape(BATCH, NEW, HEADS, DK)
        fade_log_amount = (fade_log_amount + additional_dwindle_exponent[..., None]) * live_entry_indicator[:, :, None, None]
        key_rows = key_rows.reshape(BATCH, NEW, HEADS, DK) * live_entry_indicator[:, :, None, None]
        output, updated = advance(query_rows.reshape(BATCH, NEW, HEADS, DK), key_rows, value_rows.reshape(BATCH, NEW, HEADS, DV), fade_log_amount, earlier_recurrence_grid[block_index])
        new_states.append(updated)
        normed_out = scaled_rms(output, headwise_normalizer_scales[block_index]).reshape(number_of_lines, VW)
        gated_rows = (normed_out * jax.nn.silu(gate_rows) * live_entry_indicator.reshape(number_of_lines, 1)).astype(jnp.bfloat16)
        mixed = jnp.dot(gated_rows, closing_projector[block_index], preferred_element_type=jnp.float32)
        ongoing = (ongoing.astype(jnp.float32) + mixed).astype(jnp.bfloat16)
    return (ongoing.reshape(BATCH, NEW, MODEL_BREADTH), jnp.stack(new_states, axis=0))
```

```python
import functools
import jax
import jax.numpy as jnp
from jax import lax
from jax.experimental import pallas as pl
from jax.experimental.pallas import tpu as pltpu
from jax.sharding import PartitionSpec as P

LAYERS = 2
EPS = 1e-06
TAU = 16.0
MESH = pl.DeviceIdType.MESH
F32 = jnp.float32
BF16 = jnp.bfloat16


def flip(me, bits):
    out, bit = me, 1
    while bit <= bits:
        if bits & bit:
            out = out + bit * (1 - 2 * (lax.div(me, bit) % 2))
        bit *= 2
    return out


def slots_of(n):
    table = {}
    for k in range(n.bit_length() - 1):
        for t in range(n >> (k + 1)):
            table[k, t] = len(table)
    return table


def greet(n, axis, me):
    barrier = pltpu.get_barrier_semaphore()
    steps = n.bit_length() - 1
    for k in range(steps):
        pl.semaphore_signal(barrier, inc=1, device_id={axis: flip(me, 1 << k)}, device_id_type=MESH)
    pl.semaphore_wait(barrier, steps)


def scatter_kernel(n, axis, x_ref, ss_ref, y_ref, sso_ref, rbuf, rss, sbuf, sss, send, recv, ssend, srecv):
    me = lax.axis_index(axis)
    slots = slots_of(n)
    steps = n.bit_length() - 1
    rows = x_ref.shape[1]
    piece = 16 if rows % 16 == 0 else rows
    greet(n, axis, me)
    copies = {}
    waited = set()

    def arrive(key):
        if key not in waited:
            waited.add(key)
            for c in copies[key]:
                c.wait_recv()

    for k in range(steps):
        peer = flip(me, 1 << k)
        for t in reversed(range(n >> (k + 1))):
            slot = slots[k, t]
            bits = (1 << k) | (t << (k + 1))
            chunk = flip(me, bits)
            if k == 0:
                src, ssrc = x_ref.at[chunk], ss_ref.at[chunk]
            else:
                terms = [(j, bits >> (j + 1)) for j in range(k)]
                for term in terms:
                    arrive(term)
                places = [slots[term] for term in terms]
                out = slot - slots[1, 0]

                @pl.loop(0, rows // piece)
                def _(i):
                    at = pl.ds(pl.multiple_of(i * piece, piece), piece)
                    total = x_ref[chunk, at, :].astype(F32)
                    for place in places:
                        total += rbuf[place, at, :].astype(F32)
                    sbuf[out, at, :] = total.astype(BF16)

                small = ss_ref[chunk]
                for place in places:
                    small += rss[place]
                sss[out] = small
                src, ssrc = sbuf.at[out], sss.at[out]
            pair = [
                pltpu.make_async_remote_copy(ssrc, rss.at[slot], ssend.at[slot], srecv.at[slot],
                                             device_id={axis: peer}, device_id_type=MESH),
                pltpu.make_async_remote_copy(src, rbuf.at[slot], send.at[slot], recv.at[slot],
                                             device_id={axis: peer}, device_id_type=MESH),
            ]
            for c in pair:
                c.start()
            copies[k, t] = pair
    places = [slots[k, 0] for k in range(steps)]
    for key in slots:
        arrive(key)

    @pl.loop(0, rows // piece)
    def _(i):
        at = pl.ds(pl.multiple_of(i * piece, piece), piece)
        total = x_ref[me, at, :].astype(F32)
        for place in places:
            total += rbuf[place, at, :].astype(F32)
        y_ref[at, :] = total.astype(BF16)

    small = ss_ref[me]
    for place in places:
        small += rss[place]
    sso_ref[...] = small
    for pair in copies.values():
        for c in pair:
            c.wait_send()


def reduce_scatter(n, axis, x, ss, cid):
    _, m, cols = x.shape
    count = len(slots_of(n))
    held = max(1, count - n // 2)
    vm = pl.BlockSpec(memory_space=pltpu.VMEM)
    dma = pltpu.SemaphoreType.DMA((count,))
    return pl.pallas_call(
        functools.partial(scatter_kernel, n, axis),
        out_shape=(jax.ShapeDtypeStruct((m, cols), BF16), jax.ShapeDtypeStruct((1, m), F32)),
        in_specs=[vm, vm],
        out_specs=(vm, vm),
        scratch_shapes=[
            pltpu.VMEM((count, m, cols), BF16), pltpu.VMEM((count, 1, m), F32),
            pltpu.VMEM((held, m, cols), BF16), pltpu.VMEM((held, 1, m), F32),
            dma, dma, dma, dma,
        ],
        compiler_params=pltpu.CompilerParams(collective_id=cid, has_side_effects=True),
    )(x, ss)


def gather_kernel(n, axis, g_ref, live_ref, o_ref, lo_ref, buf, lbuf, send, recv, lsend, lrecv):
    me = lax.axis_index(axis)
    slots = slots_of(n)
    steps = n.bit_length() - 1
    greet(n, axis, me)
    copies = {}

    def push(k, bits):
        t = bits >> (k + 1)
        slot = slots[k, t]
        chunk = flip(me, bits)
        src = g_ref if bits == 0 else buf.at[chunk]
        lsrc = live_ref if bits == 0 else lbuf.at[chunk]
        peer = {axis: flip(me, 1 << k)}
        pair = [
            pltpu.make_async_remote_copy(lsrc, lbuf.at[chunk], lsend.at[slot], lrecv.at[slot],
                                         device_id=peer, device_id_type=MESH),
            pltpu.make_async_remote_copy(src, buf.at[chunk], send.at[slot], recv.at[slot],
                                         device_id=peer, device_id_type=MESH),
        ]
        for c in pair:
            c.start()
        copies[k, t] = pair

    for k in reversed(range(steps)):
        push(k, 0)
    o_ref[me] = g_ref[...]
    lo_ref[me] = live_ref[...]
    for k in reversed(range(steps)):
        for t in range(n >> (k + 1)):
            for c in copies[k, t]:
                c.wait_recv()
            bits = (1 << k) | (t << (k + 1))
            for j in reversed(range(k)):
                push(j, bits)
            chunk = flip(me, bits)
            o_ref[chunk] = buf[chunk]
            lo_ref[chunk] = lbuf[chunk]
    for pair in copies.values():
        for c in pair:
            c.wait_send()


def all_gather(n, axis, g, live, cid):
    m, cols = g.shape
    count = len(slots_of(n))
    vm = pl.BlockSpec(memory_space=pltpu.VMEM)
    dma = pltpu.SemaphoreType.DMA((count,))
    return pl.pallas_call(
        functools.partial(gather_kernel, n, axis),
        out_shape=(jax.ShapeDtypeStruct((n, m, cols), BF16), jax.ShapeDtypeStruct((n, 1, m), F32)),
        in_specs=[vm, vm],
        out_specs=(vm, vm),
        scratch_shapes=[pltpu.VMEM((n, m, cols), BF16), pltpu.VMEM((n, 1, m), F32), dma, dma, dma, dma],
        compiler_params=pltpu.CompilerParams(collective_id=cid, has_side_effects=True),
    )(g, live)


def shift_rows(x, d):
    return x if d == 0 else pltpu.roll(x, d, 0)


def recurrence_kernel(heads, dk, dv, new, y_ref, scale_ref, live_ref, bias_ref, extra_ref, gain_ref, s_ref, *rest):
    g_ref, out_ref = rest[-2:]
    rows = y_ref.shape[0]
    seqs = rows // new
    kc, vc = heads * dk, heads * dv
    scale = scale_ref[...]
    live = live_ref[...]
    slot = lax.broadcasted_iota(jnp.int32, (rows, 1), 0) % new
    rowid = lax.broadcasted_iota(jnp.int32, (rows, 1), 0) // new
    for h in range(heads):
        ks, vs = pl.ds(h * dk, dk), h * dv
        q = y_ref[:, h * dk:(h + 1) * dk].astype(F32) * (scale * dk ** -0.5)
        k = y_ref[:, kc + h * dk:kc + (h + 1) * dk].astype(F32) * (scale * live)
        v = y_ref[:, 2 * kc + vs:2 * kc + vs + dv].astype(F32) * scale
        r = y_ref[:, 2 * kc + vc + vs:2 * kc + vc + vs + dv].astype(F32) * scale
        logit = y_ref[:, 2 * kc + 2 * vc + h * dk:2 * kc + 2 * vc + (h + 1) * dk].astype(F32) * scale
        z = logit + bias_ref[0, :, ks]
        logsig = jnp.minimum(z, 0.0) - jnp.log1p(jnp.exp(-jnp.abs(z)))
        a = (logsig / TAU + extra_ref[:, h:h + 1]) * live
        c, d = a, 1
        while d < new:
            c = c + jnp.where(slot >= d, shift_rows(c, d), 0.0)
            d *= 2
        last = c.reshape(seqs, new, dk)[:, new - 1:new, :]
        last = jnp.broadcast_to(last, (seqs, new, dk)).reshape(rows, dk)
        o = jnp.zeros((rows, dv), F32)
        for d in range(new):
            ok = slot >= d
            gap = jnp.where(ok, c - shift_rows(c, d), 0.0)
            s = jnp.sum(q * shift_rows(k, d) * jnp.exp(gap), axis=1, keepdims=True)
            o = o + jnp.where(ok, s, 0.0) * shift_rows(v, d)
        qe = (q * jnp.exp(c)).astype(BF16)
        ke = (k * jnp.exp(last - c)).T.astype(BF16)
        el = jnp.exp(last).T
        parts = []
        for i in range(seqs):
            state = s_ref[0, i, h]
            parts.append(jnp.dot(qe[i * new:(i + 1) * new], state.astype(BF16), preferred_element_type=F32))
            vm = jnp.where(rowid == i, v, 0.0).astype(BF16)
            upd = jnp.dot(ke, vm, preferred_element_type=F32)
            out_ref[0, i, h] = el[:, i * new:i * new + 1] * state + upd
        o = o + jnp.concatenate(parts, axis=0)
        norm = o * lax.rsqrt(jnp.mean(o * o, axis=1, keepdims=True) + EPS) * gain_ref[0].astype(F32)
        g_ref[:, vs:vs + dv] = (norm * (r * jax.nn.sigmoid(r)) * live).astype(BF16)


def recurrence(layer, y, scale, live, bias, extra, gains, grid, states):
    layers, seqs, heads, dk, dv = grid.shape
    new = y.shape[0] // seqs
    block = 4 if seqs % 4 == 0 else 1
    rows = block * new
    cols = y.shape[1]
    by_row = lambda width: pl.BlockSpec((rows, width), lambda b: (b, 0))
    state_spec = pl.BlockSpec((1, block, heads, dk, dv), lambda b: (layer, b, 0, 0, 0))
    args = [y, scale, live, bias.reshape(layers, 1, -1), extra, gains.reshape(layers, 1, -1), grid]
    in_specs = [
        by_row(cols), by_row(1), by_row(1),
        pl.BlockSpec((1, 1, heads * dk), lambda b: (layer, 0, 0)),
        by_row(heads),
        pl.BlockSpec((1, 1, dv), lambda b: (layer, 0, 0)),
        state_spec,
    ]
    alias = {}
    if states is not None:
        args.append(states)
        in_specs.append(pl.BlockSpec(memory_space=pl.ANY))
        alias = {len(args) - 1: 1}
    return pl.pallas_call(
        functools.partial(recurrence_kernel, heads, dk, dv, new),
        grid=(seqs // block,),
        out_shape=(jax.ShapeDtypeStruct((seqs * new, heads * dv), BF16), jax.ShapeDtypeStruct(grid.shape, F32)),
        in_specs=in_specs,
        out_specs=(by_row(heads * dv), state_spec),
        input_output_aliases=alias,
        compiler_params=pltpu.CompilerParams(dimension_semantics=("arbitrary",)),
    )(*args)


def shards(x0, lengths, norm_gains, wq, wk, wv, wr, wa, bias, extra, head_gains, wo, grid):
    streams, new, width = x0.shape
    lines = streams * new
    seqs = lengths.shape[0]
    rows = seqs * new
    n = lines // rows
    full = width * n
    x = x0.reshape(lines, width)
    live = (lax.broadcasted_iota(jnp.int32, (seqs, new), 1) < lengths[:, None]).astype(F32)
    live_col, live_row = live.reshape(rows, 1), live.reshape(1, rows)
    extra = extra.reshape(rows, -1)
    states = None
    for l in range(LAYERS):
        xf = x.astype(F32)
        ss = jnp.sum(xf * xf, axis=1).reshape(n, 1, rows)
        scaled = (xf * norm_gains[l].astype(F32)).astype(BF16)
        partial = jnp.concatenate(
            [jnp.dot(scaled, w[l], preferred_element_type=F32).astype(BF16) for w in (wq, wk, wv, wr, wa)], axis=1)
        y, total = reduce_scatter(n, "dp", partial.reshape(n, rows, -1), ss, 2 * l)
        scale = lax.rsqrt(total / full + EPS).reshape(rows, 1)
        g, states = recurrence(l, y, scale, live_col, bias, extra, head_gains, grid, states)
        every, alive = all_gather(n, "dp", g, live_row, 2 * l + 1)
        alive = alive.reshape(1, lines)
        rank = jnp.cumsum(alive, axis=1) - 1.0
        index = lax.broadcasted_iota(jnp.int32, (lines // 2, lines), 0).astype(F32)
        pick = ((rank == index) & (alive > 0)).astype(BF16)
        packed = jnp.dot(pick, every.reshape(lines, -1), preferred_element_type=F32).astype(BF16)
        mixed = lax.psum(jnp.dot(packed, wo[l], preferred_element_type=F32).astype(BF16), "tp")
        spread = lax.dot_general(pick, mixed, (((0,), (0,)), ((), ())), preferred_element_type=F32)
        x = (xf + spread).astype(BF16)
    return x.reshape(streams, new, width), states


def solution(mesh):
    in_specs = (
        P("grp", None, "dp"),
        P(("grp", "dp")),
        P(None, "dp"),
        P(None, "dp", "tp"),
        P(None, "dp", "tp"),
        P(None, "dp", "tp"),
        P(None, "dp", "tp"),
        P(None, "dp", "tp"),
        P(None, "tp"),
        P(("grp", "dp"), None, "tp"),
        P(),
        P(None, "tp", "dp"),
        P(None, ("grp", "dp"), "tp", None, None),
    )
    out_specs = (P("grp", None, "dp"), P(None, ("grp", "dp"), "tp", None, None))
    return jax.shard_map(shards, mesh=mesh, in_specs=in_specs, out_specs=out_specs, check_vma=False)
```

```python
import functools
import jax
import jax.numpy as jnp
from jax import lax
from jax.experimental import pallas as pl
from jax.experimental.pallas import tpu as pltpu
from jax.sharding import PartitionSpec as P

LAYERS = 2
EPS = 1e-06
TAU = 16.0
MESH = pl.DeviceIdType.MESH
F32 = jnp.float32
BF16 = jnp.bfloat16


def flip(me, bits):
    out, bit = me, 1
    while bit <= bits:
        if bits & bit:
            out = out + bit * (1 - 2 * (lax.div(me, bit) % 2))
        bit *= 2
    return out


def slots_of(n):
    table = {}
    for k in range(n.bit_length() - 1):
        for t in range(n >> (k + 1)):
            table[k, t] = len(table)
    return table


def greet(n, axis, me):
    barrier = pltpu.get_barrier_semaphore()
    steps = n.bit_length() - 1
    for k in range(steps):
        pl.semaphore_signal(barrier, inc=1, device_id={axis: flip(me, 1 << k)}, device_id_type=MESH)
    pl.semaphore_wait(barrier, steps)


def scatter_kernel(n, axis, x_ref, ss_ref, y_ref, sso_ref, rbuf, rss, sbuf, sss, send, recv, ssend, srecv):
    me = lax.axis_index(axis)
    slots = slots_of(n)
    steps = n.bit_length() - 1
    rows = x_ref.shape[1]
    piece = 16 if rows % 16 == 0 else rows
    greet(n, axis, me)
    copies = {}
    waited = set()

    def arrive(key):
        if key not in waited:
            waited.add(key)
            for c in copies[key]:
                c.wait_recv()

    for k in range(steps):
        peer = flip(me, 1 << k)
        for t in reversed(range(n >> (k + 1))):
            slot = slots[k, t]
            bits = (1 << k) | (t << (k + 1))
            chunk = flip(me, bits)
            if k == 0:
                src, ssrc = x_ref.at[chunk], ss_ref.at[chunk]
            else:
                terms = [(j, bits >> (j + 1)) for j in range(k)]
                for term in terms:
                    arrive(term)
                places = [slots[term] for term in terms]
                out = slot - slots[1, 0]

                @pl.loop(0, rows // piece)
                def _(i):
                    at = pl.ds(pl.multiple_of(i * piece, piece), piece)
                    total = x_ref[chunk, at, :].astype(F32)
                    for place in places:
                        total += rbuf[place, at, :].astype(F32)
                    sbuf[out, at, :] = total.astype(BF16)

                small = ss_ref[chunk]
                for place in places:
                    small += rss[place]
                sss[out] = small
                src, ssrc = sbuf.at[out], sss.at[out]
            pair = [
                pltpu.make_async_remote_copy(ssrc, rss.at[slot], ssend.at[slot], srecv.at[slot],
                                             device_id={axis: peer}, device_id_type=MESH),
                pltpu.make_async_remote_copy(src, rbuf.at[slot], send.at[slot], recv.at[slot],
                                             device_id={axis: peer}, device_id_type=MESH),
            ]
            for c in pair:
                c.start()
            copies[k, t] = pair
    places = [slots[k, 0] for k in range(steps)]
    for key in slots:
        arrive(key)

    @pl.loop(0, rows // piece)
    def _(i):
        at = pl.ds(pl.multiple_of(i * piece, piece), piece)
        total = x_ref[me, at, :].astype(F32)
        for place in places:
            total += rbuf[place, at, :].astype(F32)
        y_ref[at, :] = total.astype(BF16)

    small = ss_ref[me]
    for place in places:
        small += rss[place]
    sso_ref[...] = small
    for pair in copies.values():
        for c in pair:
            c.wait_send()


def reduce_scatter(n, axis, x, ss, cid):
    _, m, cols = x.shape
    count = len(slots_of(n))
    held = max(1, count - n // 2)
    vm = pl.BlockSpec(memory_space=pltpu.VMEM)
    dma = pltpu.SemaphoreType.DMA((count,))
    return pl.pallas_call(
        functools.partial(scatter_kernel, n, axis),
        out_shape=(jax.ShapeDtypeStruct((m, cols), BF16), jax.ShapeDtypeStruct(ss.shape[1:], F32)),
        in_specs=[vm, vm],
        out_specs=(vm, vm),
        scratch_shapes=[
            pltpu.VMEM((count, m, cols), BF16), pltpu.VMEM((count,) + ss.shape[1:], F32),
            pltpu.VMEM((held, m, cols), BF16), pltpu.VMEM((held,) + ss.shape[1:], F32),
            dma, dma, dma, dma,
        ],
        compiler_params=pltpu.CompilerParams(collective_id=cid, has_side_effects=True),
    )(x, ss)


def project_kernel(n, axis, layer, plan, h_ref, ss_ref, *rest):
    weights = rest[:5]
    y_ref, sso_ref, wbuf, xbuf, rbuf, rss, sbuf, sss, load, send, recv, ssend, srecv = rest[5:]
    me = lax.axis_index(axis)
    slots = slots_of(n)
    steps = n.bit_length() - 1
    segs, wide = len(plan), wbuf.shape[2]
    loads = []
    for s, (which, start) in enumerate(plan):
        c = pltpu.make_async_copy(weights[which].at[layer, :, pl.ds(start, wide)], wbuf.at[s], load.at[s])
        c.start()
        loads.append(c)
    greet(n, axis, me)
    copies = {}
    waited = set()

    def arrive(key):
        if key not in waited:
            waited.add(key)
            for c in copies[key]:
                c.wait_recv()

    def step(k, s):
        peer = {axis: flip(me, 1 << k)}
        for t in reversed(range(n >> (k + 1))):
            slot = slots[k, t]
            bits = (1 << k) | (t << (k + 1))
            chunk = flip(me, bits)
            if k == 0:
                src, ssrc = xbuf.at[s, chunk], ss_ref.at[chunk]
            else:
                terms = [(j, bits >> (j + 1)) for j in range(k)]
                out = slot - slots[1, 0]
                total = xbuf[s, chunk].astype(F32)
                for term in terms:
                    arrive(term + (s,))
                    total += rbuf[slots[term], s].astype(F32)
                sbuf[out, s] = total.astype(BF16)
                src, ssrc = sbuf.at[out, s], sss.at[out]
                if s == 0:
                    small = ss_ref[chunk]
                    for term in terms:
                        small += rss[slots[term]]
                    sss[out] = small
            group = []
            if s == 0:
                group.append(pltpu.make_async_remote_copy(
                    ssrc, rss.at[slot], ssend.at[slot], srecv.at[slot], device_id=peer, device_id_type=MESH))
            group.append(pltpu.make_async_remote_copy(
                src, rbuf.at[slot, s], send.at[slot, s], recv.at[slot, s], device_id=peer, device_id_type=MESH))
            for c in group:
                c.start()
            copies[k, t, s] = group

    for turn in range(segs + steps - 1):
        if turn < segs:
            loads[turn].wait()

            @pl.loop(0, n)
            def _(i):
                xbuf[turn, i] = jnp.dot(h_ref[i], wbuf[turn], preferred_element_type=F32).astype(BF16)

            step(0, turn)
        for k in range(1, steps):
            if 0 <= turn - k < segs:
                step(k, turn - k)
    for s in range(segs):
        total = xbuf[s, me].astype(F32)
        for k in range(steps):
            arrive((k, 0, s))
            total += rbuf[slots[k, 0], s].astype(F32)
        y_ref[:, s * wide:(s + 1) * wide] = total.astype(BF16)
    small = ss_ref[me]
    for k in range(steps):
        small += rss[slots[k, 0]]
    sso_ref[...] = small
    for key, group in copies.items():
        arrive(key)
        for c in group:
            c.wait_send()


def project_scatter(n, axis, layer, h, ss, weights, cid):
    _, m, depth = h.shape
    wide = min(w.shape[2] for w in weights)
    plan = [(i, c) for i, w in enumerate(weights) for c in range(0, w.shape[2], wide)]
    segs = len(plan)
    count = len(slots_of(n))
    held = max(1, count - n // 2)
    vm = pl.BlockSpec(memory_space=pltpu.VMEM)
    dma = lambda *shape: pltpu.SemaphoreType.DMA(shape)
    return pl.pallas_call(
        functools.partial(project_kernel, n, axis, layer, plan),
        out_shape=(jax.ShapeDtypeStruct((m, segs * wide), BF16), jax.ShapeDtypeStruct((1, m), F32)),
        in_specs=[vm, vm] + [pl.BlockSpec(memory_space=pl.ANY)] * 5,
        out_specs=(vm, vm),
        scratch_shapes=[
            pltpu.VMEM((segs, depth, wide), BF16),
            pltpu.VMEM((segs, n, m, wide), BF16),
            pltpu.VMEM((count, segs, m, wide), BF16), pltpu.VMEM((count, 1, m), F32),
            pltpu.VMEM((held, segs, m, wide), BF16), pltpu.VMEM((held, 1, m), F32),
            dma(segs), dma(count, segs), dma(count, segs), dma(count), dma(count),
        ],
        compiler_params=pltpu.CompilerParams(
            collective_id=cid, has_side_effects=True, vmem_limit_bytes=40 * 1024 * 1024),
    )(h, ss, *weights)


def gather_kernel(n, axis, g_ref, live_ref, o_ref, lo_ref, buf, lbuf, send, recv, lsend, lrecv):
    me = lax.axis_index(axis)
    slots = slots_of(n)
    steps = n.bit_length() - 1
    greet(n, axis, me)
    copies = {}

    def push(k, bits):
        t = bits >> (k + 1)
        slot = slots[k, t]
        chunk = flip(me, bits)
        src = g_ref if bits == 0 else buf.at[chunk]
        lsrc = live_ref if bits == 0 else lbuf.at[chunk]
        peer = {axis: flip(me, 1 << k)}
        pair = [
            pltpu.make_async_remote_copy(lsrc, lbuf.at[chunk], lsend.at[slot], lrecv.at[slot],
                                         device_id=peer, device_id_type=MESH),
            pltpu.make_async_remote_copy(src, buf.at[chunk], send.at[slot], recv.at[slot],
                                         device_id=peer, device_id_type=MESH),
        ]
        for c in pair:
            c.start()
        copies[k, t] = pair

    for k in reversed(range(steps)):
        push(k, 0)
    o_ref[me] = g_ref[...]
    lo_ref[me] = live_ref[...]
    for k in reversed(range(steps)):
        for t in range(n >> (k + 1)):
            for c in copies[k, t]:
                c.wait_recv()
            bits = (1 << k) | (t << (k + 1))
            for j in reversed(range(k)):
                push(j, bits)
            chunk = flip(me, bits)
            o_ref[chunk] = buf[chunk]
            lo_ref[chunk] = lbuf[chunk]
    for pair in copies.values():
        for c in pair:
            c.wait_send()


def all_gather(n, axis, g, live, cid):
    m, cols = g.shape
    count = len(slots_of(n))
    vm = pl.BlockSpec(memory_space=pltpu.VMEM)
    dma = pltpu.SemaphoreType.DMA((count,))
    return pl.pallas_call(
        functools.partial(gather_kernel, n, axis),
        out_shape=(jax.ShapeDtypeStruct((n, m, cols), BF16), jax.ShapeDtypeStruct((n,) + live.shape, F32)),
        in_specs=[vm, vm],
        out_specs=(vm, vm),
        scratch_shapes=[pltpu.VMEM((n, m, cols), BF16), pltpu.VMEM((n,) + live.shape, F32), dma, dma, dma, dma],
        compiler_params=pltpu.CompilerParams(collective_id=cid, has_side_effects=True),
    )(g, live)


def shift_rows(x, d):
    return x if d == 0 else pltpu.roll(x, d, 0)


def recurrence_kernel(heads, dk, dv, new, y_ref, scale_ref, live_ref, bias_ref, extra_ref, gain_ref, s_ref, *rest):
    g_ref, out_ref = rest[-2:]
    rows = y_ref.shape[0]
    seqs = rows // new
    kc, vc = heads * dk, heads * dv
    scale = scale_ref[...]
    live = live_ref[...]
    slot = lax.broadcasted_iota(jnp.int32, (rows, 1), 0) % new
    rowid = lax.broadcasted_iota(jnp.int32, (rows, 1), 0) // new
    for h in range(heads):
        ks, vs = pl.ds(h * dk, dk), h * dv
        q = y_ref[:, h * dk:(h + 1) * dk].astype(F32) * (scale * dk ** -0.5)
        k = y_ref[:, kc + h * dk:kc + (h + 1) * dk].astype(F32) * (scale * live)
        v = y_ref[:, 2 * kc + vs:2 * kc + vs + dv].astype(F32) * scale
        r = y_ref[:, 2 * kc + vc + vs:2 * kc + vc + vs + dv].astype(F32) * scale
        logit = y_ref[:, 2 * kc + 2 * vc + h * dk:2 * kc + 2 * vc + (h + 1) * dk].astype(F32) * scale
        z = logit + bias_ref[0, :, ks]
        logsig = jnp.minimum(z, 0.0) - jnp.log1p(jnp.exp(-jnp.abs(z)))
        a = (logsig / TAU + extra_ref[:, h:h + 1]) * live
        c, d = a, 1
        while d < new:
            c = c + jnp.where(slot >= d, shift_rows(c, d), 0.0)
            d *= 2
        last = c.reshape(seqs, new, dk)[:, new - 1:new, :]
        last = jnp.broadcast_to(last, (seqs, new, dk)).reshape(rows, dk)
        o = jnp.zeros((rows, dv), F32)
        for d in range(new):
            ok = slot >= d
            gap = jnp.where(ok, c - shift_rows(c, d), 0.0)
            s = jnp.sum(q * shift_rows(k, d) * jnp.exp(gap), axis=1, keepdims=True)
            o = o + jnp.where(ok, s, 0.0) * shift_rows(v, d)
        qe = (q * jnp.exp(c)).astype(BF16)
        ke = (k * jnp.exp(last - c)).T.astype(BF16)
        el = jnp.exp(last).T
        parts = []
        for i in range(seqs):
            state = s_ref[0, i, h]
            parts.append(jnp.dot(qe[i * new:(i + 1) * new], state.astype(BF16), preferred_element_type=F32))
            vm = jnp.where(rowid == i, v, 0.0).astype(BF16)
            upd = jnp.dot(ke, vm, preferred_element_type=F32)
            out_ref[0, i, h] = el[:, i * new:i * new + 1] * state + upd
        o = o + jnp.concatenate(parts, axis=0)
        norm = o * lax.rsqrt(jnp.mean(o * o, axis=1, keepdims=True) + EPS) * gain_ref[0].astype(F32)
        g_ref[:, vs:vs + dv] = (norm * (r * jax.nn.sigmoid(r)) * live).astype(BF16)


def recurrence(layer, y, scale, live, bias, extra, gains, grid, states):
    layers, seqs, heads, dk, dv = grid.shape
    new = y.shape[0] // seqs
    block = 4 if seqs % 4 == 0 else 1
    rows = block * new
    cols = y.shape[1]
    by_row = lambda width: pl.BlockSpec((rows, width), lambda b: (b, 0))
    state_spec = pl.BlockSpec((1, block, heads, dk, dv), lambda b: (layer, b, 0, 0, 0))
    args = [y, scale, live, bias.reshape(layers, 1, -1), extra, gains.reshape(layers, 1, -1), grid]
    in_specs = [
        by_row(cols), by_row(1), by_row(1),
        pl.BlockSpec((1, 1, heads * dk), lambda b: (layer, 0, 0)),
        by_row(heads),
        pl.BlockSpec((1, 1, dv), lambda b: (layer, 0, 0)),
        state_spec,
    ]
    alias = {}
    if states is not None:
        args.append(states)
        in_specs.append(pl.BlockSpec(memory_space=pl.ANY))
        alias = {len(args) - 1: 1}
    return pl.pallas_call(
        functools.partial(recurrence_kernel, heads, dk, dv, new),
        grid=(seqs // block,),
        out_shape=(jax.ShapeDtypeStruct((seqs * new, heads * dv), BF16), jax.ShapeDtypeStruct(grid.shape, F32)),
        in_specs=in_specs,
        out_specs=(by_row(heads * dv), state_spec),
        input_output_aliases=alias,
        compiler_params=pltpu.CompilerParams(dimension_semantics=("arbitrary",)),
    )(*args)


def shards(x0, lengths, norm_gains, wq, wk, wv, wr, wa, bias, extra, head_gains, wo, grid):
    streams, new, width = x0.shape
    lines = streams * new
    seqs = lengths.shape[0]
    rows = seqs * new
    n = lines // rows
    full = width * n
    x = x0.reshape(lines, width)
    live = (lax.broadcasted_iota(jnp.int32, (seqs, new), 1) < lengths[:, None]).astype(F32)
    live_col, live_row = live.reshape(rows, 1), live.reshape(1, rows)
    extra = extra.reshape(rows, -1)
    states = None
    for l in range(LAYERS):
        xf = x.astype(F32)
        ss = jnp.sum(xf * xf, axis=1).reshape(n, 1, rows)
        scaled = (xf * norm_gains[l].astype(F32)).astype(BF16)
        y, total = project_scatter(n, "dp", l, scaled.reshape(n, rows, width), ss, (wq, wk, wv, wr, wa), 4 * l)
        scale = lax.rsqrt(total / full + EPS).reshape(rows, 1)
        g, states = recurrence(l, y, scale, live_col, bias, extra, head_gains, grid, states)
        every, alive = all_gather(n, "dp", g, live_row, 4 * l + 1)
        alive = alive.reshape(1, lines)
        rank = jnp.cumsum(alive, axis=1) - 1.0
        index = lax.broadcasted_iota(jnp.int32, (lines // 2, lines), 0).astype(F32)
        pick = ((rank == index) & (alive > 0)).astype(BF16)
        packed = jnp.dot(pick, every.reshape(lines, -1), preferred_element_type=F32).astype(BF16)
        part = jnp.dot(packed, wo[l], preferred_element_type=F32).astype(BF16)
        heads_n = lax.axis_size("tp")
        spare = jnp.zeros((heads_n, 1, 128), F32)
        mine, word = reduce_scatter(heads_n, "tp", part.reshape(heads_n, -1, width), spare, 4 * l + 2)
        mixed, _ = all_gather(heads_n, "tp", mine, word, 4 * l + 3)
        mixed = mixed.reshape(-1, width)
        spread = lax.dot_general(pick, mixed, (((0,), (0,)), ((), ())), preferred_element_type=F32)
        x = (xf + spread).astype(BF16)
    return x.reshape(streams, new, width), states


def solution(mesh):
    in_specs = (
        P("grp", None, "dp"),
        P(("grp", "dp")),
        P(None, "dp"),
        P(None, "dp", "tp"),
        P(None, "dp", "tp"),
        P(None, "dp", "tp"),
        P(None, "dp", "tp"),
        P(None, "dp", "tp"),
        P(None, "tp"),
        P(("grp", "dp"), None, "tp"),
        P(),
        P(None, "tp", "dp"),
        P(None, ("grp", "dp"), "tp", None, None),
    )
    out_specs = (P("grp", None, "dp"), P(None, ("grp", "dp"), "tp", None, None))
    return jax.shard_map(shards, mesh=mesh, in_specs=in_specs, out_specs=out_specs, check_vma=False)
```
